256 devices in a mesh: sp: 16 (over y, x), tp: 16 (over z, core).
Axes of the slice: x: 4, y: 4, z: 8, core: 2. Of those that a mesh axis runs over, the one named last changes fastest.
Arguments:
- residual_mid: bfloat16 [2560, 4096], P('sp'), may hold values from -100 to 100
- out_grad: bfloat16 [2560, 4096], P('sp'), may hold values from -6 to 6
- norm_gain: float32 [4096], replicated, may hold values from 0.1 to 1.9
- expert_ids: int32 [2560, 2], P('sp'), may hold values from 0 to 15, all different within a row; in each aligned block of 160 rows (0 to 159, 160 to 319, ...) at most 40 rows name the same one
- expert_weights: float32 [2560, 2], P('sp'), may hold values from 0.1 to 1
- gate_proj: bfloat16 [16, 4096, 2048], P('sp', None, 'tp'), may hold values from -0.25 to 0.25
- up_proj: bfloat16 [16, 4096, 2048], P('sp', None, 'tp'), may hold values from -0.25 to 0.25
- down_proj: bfloat16 [16, 2048, 4096], P('sp', 'tp'), may hold values from -0.125 to 0.125
- out_proj: bfloat16 [4096, 4096], P('tp'), may hold values from -0.09375 to 0.09375
- query_rows: bfloat16 [2560, 4096], P('sp', 'tp'), may hold values from -6 to 6
- key_rows: bfloat16 [2560, 4096], P('sp', 'tp'), may hold values from -6 to 6
- value_rows: bfloat16 [2560, 4096], P('sp', 'tp'), may hold values from -6 to 6
- retention_out: bfloat16 [2560, 4096], P('sp', 'tp'), may hold values from -6 to 6
- log_decay: float32 [2560, 16], P('sp', 'tp'), may hold values from -2 to 0
- entry_state: float32 [16, 16, 256, 256], P('sp', 'tp'), may hold values from -24 to 24
Outputs:
- gate_grad: bfloat16 [16, 4096, 2048], P('sp', None, 'tp')
- up_grad: bfloat16 [16, 4096, 2048], P('sp', None, 'tp')
- down_grad: bfloat16 [16, 2048, 4096], P('sp', 'tp')
- proj_grad: float32 [4096, 4096], P('sp', 'tp')
- query_grad: bfloat16 [2560, 4096], P('sp', 'tp')
- key_grad: bfloat16 [2560, 4096], P('sp', 'tp')
- value_grad: bfloat16 [2560, 4096], P('sp', 'tp')
The draws below stay inside these ranges and needn't reach their ends.
Inputs may be any that keep to these rules, and one draw needn't show every extreme that they name: `expert_ids`: each row names 2 different experts. Among the rows of one device, no expert is named by more than 40 rows, and in every draw some expert is named by exactly 40 rows of some device.
All inputs are finite; a program needn't handle non-finite values.
Results may differ from the reference program's by a relative error of at most 0.025.
The reference program's roundings to bfloat16 on the way count: a program that leaves them out, or rounds other values in their place, can miss the bound.
Values may be sent and summed in bfloat16 or wider, within the bound.
No kernel may reach another device: no remote copies, remote signals or barrier semaphores. Data moves between devices by JAX's collectives and lax.ppermute only.
A program may use at most 128 MiB of HBM per device.

```python
import math
import jax
import jax.numpy as jnp
import numpy as np
from jax import lax

D = 4096
FF = 2048
RETENTION_HEADS = 16
DK = 256
TOP = 2
TOK_DEV = 160
RW = 4096
EXPERTS = 16
SEGS = 16
SEQUENCE_TOKENS = 2560
CAP = 40
N_TP = 16


def draw_residual_mid(key, part):
    base_key, col_key, row_key = jax.random.split(key, 3)
    columns = jnp.exp(jax.random.uniform(col_key, (1, D), jnp.float32, 0.0, math.log(10.0)))
    rowscale = jnp.exp(jax.random.uniform(row_key, (SEQUENCE_TOKENS, 1), jnp.float32, math.log(0.3), math.log(3.0)))
    entries = jnp.clip(jax.random.normal(base_key, (SEQUENCE_TOKENS, D), jnp.float32), -6.0, 6.0)
    return (entries * columns * rowscale / 3.0).astype(jnp.bfloat16)


def draw_log_decay(key, part):
    random_keys = jax.random.split(key, 7)
    head_order = jax.random.permutation(random_keys[0], RETENTION_HEADS)
    fast_heads = head_order < RETENTION_HEADS // 2
    fast_span = jnp.exp(jax.random.uniform(random_keys[1], (RETENTION_HEADS,), jnp.float32, math.log(30.0), math.log(100.0)))
    slow_total = jax.random.uniform(random_keys[2], (RETENTION_HEADS,), jnp.float32, 0.05, 0.2) * math.log(10.0)
    decay_speed = jnp.where(fast_heads, math.log(20.0) / fast_span, slow_total / SEQUENCE_TOKENS)
    segment_multiplier = jnp.exp(jax.random.uniform(random_keys[3], (SEGS, RETENTION_HEADS), jnp.float32, math.log(0.5), math.log(2.0)))
    segment_multiplier = jnp.repeat(segment_multiplier, TOK_DEV, axis=0)
    jaggedness = jax.random.uniform(random_keys[4], (SEQUENCE_TOKENS, RETENTION_HEADS), jnp.float32, 0.5, 1.5)
    spike_position = jax.random.randint(random_keys[5], (2, 1), 0, SEQUENCE_TOKENS)
    spike_retained = jax.random.uniform(random_keys[6], (2, RETENTION_HEADS), jnp.float32, 0.5, 0.8)
    token_position = jnp.arange(SEQUENCE_TOKENS)[None, :, None]
    spike_matches = token_position == spike_position[:, :, None]
    spike_list = jnp.sum(jnp.where(spike_matches, jnp.log(spike_retained)[:, None, :], 0.0), axis=0)
    return (-decay_speed[None, :] * segment_multiplier * jaggedness + spike_list).astype(jnp.float32)


def with_spikes(values, own_key, source, target, blocks, factor):
    def block_of(position):
        return (jnp.arange(values.shape[position]) // (values.shape[position] // blocks)).reshape((-1,) + (1,) * (values.ndim - 1 - position))

    one_side = jax.random.permutation(own_key, blocks)[block_of(target)]
    other_side = (block_of(target) + blocks // 2) % blocks
    return jnp.where((block_of(source) == one_side) | (block_of(source) == other_side), factor * values, values)


def block_scale(own_key, shape, shards, least, largest):
    factor_of, own = 1.0, jax.random.fold_in(own_key, 6)
    for position, shards_of in shards:
        draws = jnp.exp(jax.random.uniform(jax.random.fold_in(own, position), (shards_of,), jnp.float32, least / len(shards), largest / len(shards)))
        factor_of = factor_of * jnp.repeat(draws, shape[position] // shards_of).reshape([-1 if axis == position else 1 for axis in range(len(shape))])
    return factor_of


def assign_block(key, own, number, rows, number_of, top, bound, slope):
    sequence = jax.random.permutation(key, number_of)
    packed, usual = portions_of(number_of, rows * top, bound, slope, True), portions_of(number_of, rows * top, bound, slope, False)
    places = jnp.arange(number_of)

    def named(lengths, offset_by):
        used = int((lengths > 0).sum())
        fixed = max(1, used // 4)
        passed = fixed + (places - fixed + offset_by * (used - fixed)) % max(1, number_of - fixed)
        return jnp.zeros((number_of,), jnp.int32).at[sequence[jnp.where(places < fixed, places, passed)]].set(jnp.asarray(lengths, jnp.int32))

    lengths = jnp.where(number % 4 == 0, named(packed, number // 4), named(usual, number - number // 4 - 1))
    mixed = jax.random.permutation(jax.random.fold_in(own, 3), number_of)
    giver, taker = mixed[0:number_of // 2 * 2:2], mixed[1:number_of // 2 * 2:2]
    room = jnp.minimum(lengths[giver] - 1, bound - lengths[taker]) // 2
    room = jnp.where((giver == sequence[0]) | (taker == sequence[0]) | (lengths[taker] == 0), 0, jnp.maximum(room, 0))
    passed = jax.random.randint(jax.random.fold_in(own, 4), (number_of // 2,), 0, 1 << 20) % (room + 1)
    lengths = lengths.at[giver].add(-passed).at[taker].add(passed)
    items = jnp.searchsorted(jnp.cumsum(lengths), jnp.arange(rows * top), side="right").astype(jnp.int32)
    listing = items.reshape(top, rows).T
    listing = listing[jax.random.permutation(jax.random.fold_in(own, 1), rows)]
    offset_by = jax.random.randint(jax.random.fold_in(own, 2), (rows, 1), 0, top)
    return jnp.take_along_axis(listing, (jnp.arange(top)[None, :] + offset_by) % top, axis=1)


def portions_of(amount, total, bound, slope, full):
    weights = [(1 << 20) // math.isqrt(grade ** slope) + 1 for grade in range(1, amount + 1)]
    largest = bound if full else min(bound, max(-(-total // amount), total * weights[0] // sum(weights)))
    least = 1 if total - largest >= amount - 1 else 0
    counts, spare = [largest] + [least] * (amount - 1), total - largest - least * (amount - 1)
    while spare > 0:
        free = [i for i in range(1, amount) if counts[i] < largest] or [i for i in range(1, amount) if counts[i] < bound]
        mass, budget = sum([weights[i] for i in free]), spare
        for i in free:
            extra = min(bound - counts[i], max(1, budget * weights[i] // mass), spare)
            counts[i] = counts[i] + extra
            spare = spare - extra
    return np.array(counts)


def centred(stream_key, extent, scale, bound, cuts=(), kind=jnp.bfloat16):
    level = block_scale(stream_key, extent, cuts, -0.22, 0.18) if cuts else 1.0
    values = jax.random.normal(stream_key, extent, jnp.float32) * scale * level
    return jnp.minimum(jnp.maximum(values, -bound), bound).astype(kind)


def bell_draw_with(stream_key, shape, scale, reach, shards, heavy, kind=jnp.bfloat16):
    result = scale * jax.random.normal(stream_key, shape, jnp.float32)
    if shards:
        result = result * block_scale(stream_key, shape, shards, -0.22, 0.18)
    return jnp.clip(with_spikes(result, jax.random.fold_in(stream_key, 3), *heavy), -reach, reach).astype(kind)


def setup_inputs(seed: int = 0) -> dict:
    keys = jax.random.split(jax.random.key(seed), 16)
    residual_mid = draw_residual_mid(jax.random.fold_in(keys[15], 71), 0)
    out_grad = bell_draw_with(keys[1], (SEQUENCE_TOKENS, D), 1.0, 6.0, ((0, 16),), (0, 1, 16, 2.0))
    norm_gain = jnp.clip(1.0 + 0.18 * jax.random.normal(keys[2], (D,), jnp.float32), 0.1, 1.9)
    expert_ids_keys = jax.random.split(jax.random.fold_in(keys[3], 1), SEQUENCE_TOKENS // TOK_DEV)
    expert_ids_turns = jax.random.permutation(jax.random.fold_in(keys[3], 3), SEQUENCE_TOKENS // TOK_DEV)
    expert_ids = jax.vmap(lambda own, number: assign_block(jax.random.fold_in(keys[3], 2), own, number, TOK_DEV, EXPERTS, TOP, CAP, 2))(expert_ids_keys, expert_ids_turns).reshape((SEQUENCE_TOKENS, TOP))
    expert_weights = jnp.clip(0.1 + 0.9 * jax.random.uniform(keys[4], (SEQUENCE_TOKENS, TOP), jnp.float32) ** block_scale(keys[4], (SEQUENCE_TOKENS, TOP), ((0, 16),), -0.2, 0.2), 0.1, 1.0)
    gate_proj = centred(keys[5], (EXPERTS, D, FF), (D // 9) ** -0.5, 0.25, ((0, 16), (2, 16)))
    up_proj = centred(keys[6], (EXPERTS, D, FF), (D // 9) ** -0.5, 0.25, ((0, 16), (2, 16)))
    down_proj = centred(keys[7], (EXPERTS, FF, D), FF ** -0.5, 0.125, ((0, 16), (1, 16)))
    out_proj = centred(keys[8], (RW, D), RW ** -0.5, 0.09375, ((0, 16),))
    query_rows = centred(keys[9], (SEQUENCE_TOKENS, RW), 1.0, 6.0, ((0, 16), (1, 16)))
    key_rows = centred(keys[10], (SEQUENCE_TOKENS, RW), 1.0, 6.0, ((0, 16), (1, 16)))
    value_rows = centred(keys[11], (SEQUENCE_TOKENS, RW), 1.0, 6.0, ((0, 16), (1, 16)))
    retention_out = centred(keys[12], (SEQUENCE_TOKENS, RW), 1.0, 6.0, ((0, 16), (1, 16)))
    log_decay = draw_log_decay(jax.random.fold_in(keys[15], 71), 0)
    entry_state = centred(keys[14], (SEGS, RETENTION_HEADS, DK, DK), 4.0, 24.0, ((0, 16), (1, 16)), jnp.float32)
    return dict(residual_mid=residual_mid, out_grad=out_grad, norm_gain=norm_gain, expert_ids=expert_ids, expert_weights=expert_weights, gate_proj=gate_proj, up_proj=up_proj, down_proj=down_proj, out_proj=out_proj, query_rows=query_rows, key_rows=key_rows, value_rows=value_rows, retention_out=retention_out, log_decay=log_decay, entry_state=entry_state)


CLAMP_LIMIT = 7.0
GATE_ALPHA = 1.702
NORM_EPSILON = 1e-05

def activate(gate_pre, up_pre):
    gate_clamped = jnp.minimum(gate_pre, CLAMP_LIMIT)
    up_clamped = jnp.clip(up_pre, -CLAMP_LIMIT, CLAMP_LIMIT)
    return (up_clamped + 1.0) * gate_clamped * jax.nn.sigmoid(GATE_ALPHA * gate_clamped)

def reference(residual_mid, out_grad, norm_gain, expert_ids, expert_weights, gate_proj, up_proj, down_proj, out_proj, query_rows, key_rows, value_rows, retention_out, log_decay, entry_state):
    top_count = expert_ids.shape[1]
    width = residual_mid.shape[1]
    pair_count = SEQUENCE_TOKENS * top_count
    mid_rows = residual_mid.astype(jnp.float32)
    inverse = lax.rsqrt(lax.optimization_barrier(jnp.mean(mid_rows * mid_rows, axis=1, keepdims=True)) + NORM_EPSILON)
    scaled = mid_rows * inverse
    normed = (scaled * norm_gain).astype(jnp.bfloat16)
    flat_ids = expert_ids.reshape(SEGS, TOK_DEV * top_count).astype(jnp.int32)
    chosen = (flat_ids[:, :, None] == jnp.arange(EXPERTS, dtype=jnp.int32)[None, None, :]).astype(jnp.int32)
    placed = lax.optimization_barrier(jnp.sum((jnp.cumsum(chosen, axis=1) - chosen) * chosen, axis=2)).astype(jnp.int32)
    segment = jnp.broadcast_to(jnp.arange(SEGS, dtype=jnp.int32)[:, None], flat_ids.shape)
    pair_index = jnp.arange(pair_count, dtype=jnp.int32).reshape(SEGS, TOK_DEV * top_count)
    slot_pair = jnp.full((EXPERTS, SEGS, CAP), pair_count, jnp.int32).at[flat_ids, segment, placed].set(pair_index)
    blank = jnp.zeros((1, width), jnp.bfloat16)
    token_table = jnp.concatenate([jnp.repeat(normed, top_count, axis=0), blank], axis=0)
    pair_grads = (expert_weights[:, :, None] * out_grad[:, None, :]).astype(jnp.bfloat16).reshape(pair_count, width)
    grad_table = jnp.concatenate([pair_grads, blank], axis=0)
    group_width = FF // N_TP

    def one_expert(operands):
        slot_rows, gate_weight, up_weight, down_weight = operands
        slot_index = slot_rows.reshape(-1)
        rows_in = token_table[slot_index]
        rows_grad = grad_table[slot_index]
        gate_pre = jnp.dot(rows_in, gate_weight, preferred_element_type=jnp.float32)
        up_pre = jnp.dot(rows_in, up_weight, preferred_element_type=jnp.float32)
        hidden, pullback = jax.vjp(activate, gate_pre, up_pre)
        down_part = jnp.dot(hidden.astype(jnp.bfloat16).T, rows_grad, preferred_element_type=jnp.float32).astype(jnp.bfloat16)
        hidden_grad = jnp.dot(rows_grad, down_weight.T, preferred_element_type=jnp.float32)
        gate_back, up_back = pullback(hidden_grad)
        gate_back = gate_back.astype(jnp.bfloat16)
        up_back = up_back.astype(jnp.bfloat16)
        gate_part = jnp.dot(rows_in.T, gate_back, preferred_element_type=jnp.float32).astype(jnp.bfloat16)
        up_part = jnp.dot(rows_in.T, up_back, preferred_element_type=jnp.float32).astype(jnp.bfloat16)
        row_total = rows_in.shape[0]
        parts = jnp.einsum('rjf,djf->jrd', gate_back.astype(jnp.float32).reshape(row_total, N_TP, group_width), gate_weight.astype(jnp.float32).reshape(width, N_TP, group_width))
        parts = parts + jnp.einsum('rjf,djf->jrd', up_back.astype(jnp.float32).reshape(row_total, N_TP, group_width), up_weight.astype(jnp.float32).reshape(width, N_TP, group_width))
        rounded = lax.optimization_barrier(parts.astype(jnp.bfloat16))
        summed = lax.optimization_barrier(jnp.sum(rounded.astype(jnp.float32), axis=0)).astype(jnp.bfloat16)
        return (gate_part, up_part, down_part, summed)
    gate_grad, up_grad, down_grad, returned = lax.map(one_expert, (slot_pair, gate_proj, up_proj, down_proj))
    picked = returned[flat_ids, segment * CAP + placed]
    mixed_grad = lax.optimization_barrier(jnp.sum(picked.reshape(SEQUENCE_TOKENS, top_count, width).astype(jnp.float32), axis=1))
    weighted = norm_gain * mixed_grad
    inner = lax.optimization_barrier(jnp.mean(scaled * weighted, axis=1, keepdims=True))
    resid_grad = (out_grad.astype(jnp.float32) + inverse * (weighted - scaled * inner)).astype(jnp.bfloat16)
    proj_grad = jnp.dot(resid_grad.T, retention_out, preferred_element_type=jnp.float32)
    head_grad = jnp.dot(resid_grad, out_proj.T, preferred_element_type=jnp.float32)
    heads = log_decay.shape[1]
    highest = lax.Precision.HIGHEST

    def split_heads(rows):
        return rows.astype(jnp.float32).reshape(SEGS, TOK_DEV, heads, -1).transpose(0, 2, 1, 3)
    queries = split_heads(query_rows)
    key_heads = split_heads(key_rows)
    value_heads = split_heads(value_rows)
    grad_heads = split_heads(head_grad)
    key_scale = queries.shape[3] ** (-0.5)
    running = jnp.cumsum(log_decay.reshape(SEGS, TOK_DEV, heads), axis=1).transpose(0, 2, 1)
    from_start = jnp.exp(running)
    to_end = jnp.exp(running[:, :, -1:] - running)
    token_position = jnp.arange(TOK_DEV, dtype=jnp.int32)
    causal = (token_position[:, None] >= token_position[None, :])[None, None]
    spread = jnp.where(causal, running[:, :, :, None] - running[:, :, None, :], 0.0)
    weights = jnp.where(causal, jnp.exp(spread), 0.0)
    local_state = jnp.einsum('ght,ghtk,ghte->ghke', from_start, queries, grad_heads, precision=highest)
    carry_rate = from_start[:, :, -1]

    def backward_step(carried, inputs):
        rate_now, local_now = inputs
        return (local_now + rate_now[:, None, None] * carried, carried)
    later_state = lax.scan(backward_step, jnp.zeros(local_state.shape[1:], jnp.float32), (carry_rate, local_state), reverse=True)[1]
    grad_scores = jnp.einsum('ghte,ghse->ghts', grad_heads, value_heads, precision=highest) * weights
    key_scores = jnp.einsum('ghtk,ghsk->ghts', queries, key_heads, precision=highest) * weights
    query_grad = key_scale * (jnp.einsum('ghts,ghsk->ghtk', grad_scores, key_heads, precision=highest) + from_start[..., None] * jnp.einsum('ghte,ghke->ghtk', grad_heads, entry_state, precision=highest))
    key_grad = key_scale * (jnp.einsum('ghts,ghtk->ghsk', grad_scores, queries, precision=highest) + to_end[..., None] * jnp.einsum('ghse,ghke->ghsk', value_heads, later_state, precision=highest))
    value_grad = key_scale * (jnp.einsum('ghts,ghte->ghse', key_scores, grad_heads, precision=highest) + to_end[..., None] * jnp.einsum('ghsk,ghke->ghse', key_heads, later_state, precision=highest))

    def merge_heads(heads_rows):
        return heads_rows.transpose(0, 2, 1, 3).reshape(SEQUENCE_TOKENS, -1).astype(jnp.bfloat16)
    return (gate_grad, up_grad, down_grad, proj_grad, merge_heads(query_grad), merge_heads(key_grad), merge_heads(value_grad))
```

```python
import jax
import jax.numpy as jnp
from jax import lax
from jax.experimental import pallas as pl
from jax.experimental.pallas import tpu as pltpu
from jax.sharding import Mesh
from jax.sharding import PartitionSpec as P

SP = ("y", "x")
TP = ("z", "c")
BF = jnp.bfloat16
F32 = jnp.float32

CLAMP_LIMIT = 7.0
GATE_ALPHA = 1.702
NORM_EPSILON = 1e-05


NEAR = (0, 1, 7, 2, 6)
FAR = (3, 4, 5)


def dot(a, b, ca, cb):
    return lax.dot_general(a, b, (((ca,), (cb,)), ((), ())), preferred_element_type=F32)


def along_z(a, step):
    n = lax.axis_size("z")
    return lax.ppermute(a, "z", [(i, (i + step) % n) for i in range(n)])


def partner(a):
    return lax.ppermute(a, "c", [(0, 1), (1, 0)])


def activate(gate_pre, up_pre):
    gate_clamped = jnp.minimum(gate_pre, CLAMP_LIMIT)
    up_clamped = jnp.clip(up_pre, -CLAMP_LIMIT, CLAMP_LIMIT)
    sig = jax.nn.sigmoid(GATE_ALPHA * gate_clamped)
    return gate_clamped, up_clamped, sig


VMEM = pl.BlockSpec(memory_space=pltpu.VMEM)
SMEM = pl.BlockSpec(memory_space=pltpu.SMEM)


def add_chunks(ids, refs, places, gate_ref, up_ref, down_ref, pre, back):
    fw = 256
    for ref, lane, slot in places:
        off = pl.multiple_of(ids[slot] * fw, fw)
        x = refs[ref][:, lane : lane + fw]
        g = refs[ref][:, lane + fw : lane + 2 * fw]
        w = jnp.concatenate([gate_ref[pl.ds(off, fw), :], up_ref[pl.ds(off, fw), :]], axis=1)
        pre = pre + dot(x, w, 1, 0)
        back = back + dot(g, down_ref[:, pl.ds(off, fw)], 1, 1)
    return pre, back


def first_chunks(blocks, arrays, places, gate, up, down):
    rows, hid = arrays[0].shape[0], gate.shape[1]
    n = len(arrays)

    def body(ids, *refs):
        gate_ref, up_ref, down_ref = refs[n : n + 3]
        pre_ref, back_ref = refs[n + 3 :]
        pre, back = add_chunks(
            ids, refs, places, gate_ref, up_ref, down_ref,
            jnp.zeros((rows, 2 * hid), F32), jnp.zeros((rows, hid), F32),
        )
        pre_ref[...] = pre
        back_ref[...] = back

    return pl.pallas_call(
        body,
        out_shape=(
            jax.ShapeDtypeStruct((rows, 2 * hid), F32),
            jax.ShapeDtypeStruct((rows, hid), F32),
        ),
        in_specs=[SMEM] + [VMEM] * (n + 3),
        out_specs=(VMEM, VMEM),
        name="first_chunks",
    )(blocks, *arrays, gate, up, down)


def last_chunks(blocks, arrays, places, gate, up, down, pre, back, order):
    rows, hid = arrays[0].shape[0], gate.shape[1]
    n = len(arrays)
    fw = 256

    def body(ids, *refs):
        gate_ref, up_ref, down_ref, pre_in, back_in = refs[n : n + 5]
        backs_ref, hidden_ref, own_ref, other_ref = refs[n + 5 :]
        pre, back = add_chunks(
            ids, refs, places, gate_ref, up_ref, down_ref, pre_in[...], back_in[...]
        )
        gate_pre, up_pre = pre[:, :hid], pre[:, hid:]
        c, u, sig = activate(gate_pre, up_pre)
        hidden_ref[...] = ((u + 1.0) * c * sig).astype(BF)
        slope = sig * (1.0 + GATE_ALPHA * c * (1.0 - sig))
        gate_back = jnp.where(gate_pre < CLAMP_LIMIT, back * (u + 1.0) * slope, 0.0)
        inside = (up_pre > -CLAMP_LIMIT) & (up_pre < CLAMP_LIMIT)
        up_back = jnp.where(inside, back * c * sig, 0.0)
        backs = jnp.concatenate([gate_back, up_back], axis=1).astype(BF)
        backs_ref[...] = backs
        for half, out in ((1, other_ref), (0, own_ref)):
            for i, k in enumerate(order):
                off = pl.multiple_of(ids[8 * half + k] * fw, fw)
                w = jnp.concatenate([gate_ref[pl.ds(off, fw), :], up_ref[pl.ds(off, fw), :]], axis=1)
                out[i] = dot(backs, w, 1, 1).astype(BF)

    return pl.pallas_call(
        body,
        out_shape=(
            jax.ShapeDtypeStruct((rows, 2 * hid), BF),
            jax.ShapeDtypeStruct((rows, hid), BF),
            jax.ShapeDtypeStruct((8, rows, fw), BF),
            jax.ShapeDtypeStruct((8, rows, fw), BF),
        ),
        in_specs=[SMEM] + [VMEM] * (n + 5),
        out_specs=(VMEM,) * 4,
        name="last_chunks",
    )(blocks, *arrays, gate, up, down, pre, back)


def weight_grads(blocks, arrays, places, backs, hidden):
    rows, hid = hidden.shape
    n = len(arrays)
    fw = 256
    width = fw * len(places)

    def body(ids, *refs):
        backs_ref, hidden_ref = refs[n : n + 2]
        gate_out, up_out, down_out = refs[n + 2 :]
        for ref, lane, slot in places:
            off = pl.multiple_of(ids[slot] * fw, fw)
            both = dot(refs[ref][:, lane : lane + fw], backs_ref[...], 0, 0).astype(BF)
            gate_out[pl.ds(off, fw), :] = both[:, :hid]
            up_out[pl.ds(off, fw), :] = both[:, hid:]
            g = refs[ref][:, lane + fw : lane + 2 * fw]
            down_out[:, pl.ds(off, fw)] = dot(hidden_ref[...], g, 0, 0).astype(BF)

    return pl.pallas_call(
        body,
        out_shape=(
            jax.ShapeDtypeStruct((width, hid), BF),
            jax.ShapeDtypeStruct((width, hid), BF),
            jax.ShapeDtypeStruct((hid, width), BF),
        ),
        in_specs=[SMEM] + [VMEM] * (n + 2),
        out_specs=(VMEM,) * 3,
        name="weight_grads",
    )(blocks, *arrays, backs, hidden)


def residual_grad(blocks, stacks, slots, mid, inverse, gain, out_grad, out_proj):
    rows, width = mid.shape
    n = len(stacks)
    fw = 256
    heads = out_proj.shape[0]

    def body(ids, *refs):
        mid_ref, inv_ref, gain_ref, og_ref, proj_ref = refs[n : n + 5]
        resid_ref, head_ref = refs[n + 5 :]
        inv = inv_ref[...]
        total = jnp.zeros((rows, fw), F32)
        for ref, i, slot in slots:
            off = pl.multiple_of(ids[slot] * fw, fw)
            scaled = mid_ref[:, pl.ds(off, fw)].astype(F32) * inv
            weighted = gain_ref[:, pl.ds(off, fw)] * refs[ref][i].astype(F32)
            total = total + scaled * weighted
        inner = jnp.sum(total, axis=1, keepdims=True) * (1.0 / width)
        head = jnp.zeros((rows, heads), F32)
        for ref, i, slot in slots:
            blk = ids[slot]
            off = pl.multiple_of(blk * fw, fw)
            scaled = mid_ref[:, pl.ds(off, fw)].astype(F32) * inv
            weighted = gain_ref[:, pl.ds(off, fw)] * refs[ref][i].astype(F32)
            r = og_ref[:, pl.ds(off, fw)].astype(F32) + inv * (weighted - scaled * inner)
            r = r.astype(BF)
            resid_ref[blk] = r
            head = head + dot(r, proj_ref[:, pl.ds(off, fw)], 1, 1)
        head_ref[...] = head

    return pl.pallas_call(
        body,
        out_shape=(
            jax.ShapeDtypeStruct((width // fw, rows, fw), BF),
            jax.ShapeDtypeStruct((rows, heads), F32),
        ),
        in_specs=[SMEM] + [VMEM] * (n + 5),
        out_specs=(VMEM, VMEM),
        name="residual_grad",
    )(blocks, *stacks, mid, inverse, gain, out_grad, out_proj)


def local(
    residual_mid,
    out_grad,
    norm_gain,
    expert_ids,
    expert_weights,
    gate_proj,
    up_proj,
    down_proj,
    out_proj,
    query_rows,
    key_rows,
    value_rows,
    retention_out,
    log_decay,
    entry_state,
):
    tokens, width = residual_mid.shape
    experts = 16
    capacity = 40
    slots = experts * capacity
    fw = width // 16
    half = slots // 2
    z, c = lax.axis_index("z"), lax.axis_index("c")
    seg = lax.axis_index(SP)
    rel = (z + jnp.arange(8, dtype=jnp.int32)) % 8
    blocks = jnp.concatenate([rel * 2 + c, rel * 2 + (1 - c)]).astype(jnp.int32)
    gate, up, down = gate_proj[0], up_proj[0], down_proj[0]

    names = jnp.arange(experts, dtype=jnp.int32)[None, :]
    chosen = [(expert_ids[:, k : k + 1] == names) for k in range(2)]
    named = (chosen[0] | chosen[1]).astype(BF)
    pos = jnp.arange(tokens, dtype=jnp.int32)
    earlier = (pos[:, None] > pos[None, :]).astype(BF)
    before = dot(earlier, named, 1, 0)
    slot_names = jnp.arange(slots, dtype=jnp.int32)[None, :]
    hot = []
    for k in range(2):
        place = jnp.sum(jnp.where(chosen[k], before, 0.0), axis=1, keepdims=True).astype(jnp.int32)
        hot.append((expert_ids[:, k : k + 1] * capacity + place == slot_names).astype(BF))
    hot_any = hot[0] + hot[1]

    mid_rows = residual_mid.astype(F32)
    inverse = lax.rsqrt(jnp.mean(mid_rows * mid_rows, axis=1, keepdims=True) + NORM_EPSILON)

    def share(k):
        start = blocks[k] * fw
        mid_part = lax.dynamic_slice_in_dim(residual_mid, start, fw, 1).astype(F32)
        gain_part = lax.dynamic_slice_in_dim(norm_gain, start, fw, 0)[None, :]
        grad_part = lax.dynamic_slice_in_dim(out_grad, start, fw, 1).astype(F32)
        normed = (mid_part * inverse * gain_part).astype(BF)
        pairs = [(expert_weights[:, i : i + 1] * grad_part).astype(BF) for i in range(2)]
        return normed, pairs

    def to_slots(ks):
        normed, pairs = zip(*[share(k) for k in ks])
        zero = jnp.zeros_like(normed[0])
        top = jnp.concatenate([v for n, p in zip(normed, pairs) for v in (n, p[0])], axis=1)
        low = jnp.concatenate([v for n, p in zip(normed, pairs) for v in (n, p[1])], axis=1)
        both = jnp.concatenate([hot[0], hot[1]], axis=0)
        vals = jnp.concatenate([top, low], axis=0)
        return dot(both, vals, 0, 0).astype(BF).reshape(experts, capacity, -1)

    def over_sp(a):
        return lax.all_to_all(a, SP, split_axis=0, concat_axis=0, tiled=True)

    near = over_sp(to_slots((0,))).reshape(slots, 2 * fw)
    far = over_sp(to_slots(FAR)).reshape(slots, 2 * fw * len(FAR))
    up1 = along_z(near, 1)
    dn1 = along_z(near, -1)
    up2 = along_z(up1, 1)
    dn2 = along_z(dn1, -1)
    near_o, up1_o, dn1_o = partner(near), partner(up1), partner(dn1)
    up2_o, dn2_o, far_o = partner(up2), partner(dn2), partner(far)

    first = [near, near_o, up1, up1_o, dn1, dn1_o]
    first_at = [(0, 0, 0), (1, 0, 8), (2, 0, 7), (3, 0, 15), (4, 0, 1), (5, 0, 9)]
    last = [up2, up2_o, dn2, dn2_o, far, far_o]
    last_at = [(0, 0, 6), (1, 0, 14), (2, 0, 2), (3, 0, 10)]
    for i, k in enumerate(FAR):
        last_at += [(4, 2 * fw * i, k), (5, 2 * fw * i, 8 + k)]
    pre, back = first_chunks(blocks, first, first_at, gate, up, down)
    order = (4, 3, 5, 2, 6, 1, 7, 0)
    backs, hidden, own, other = last_chunks(
        blocks, last, last_at, gate, up, down, pre, back, order
    )

    theirs = jnp.concatenate([partner(other[:3]), partner(other[3:])], axis=0)
    mine = {k: (own[i].astype(F32), theirs[i].astype(F32)) for i, k in enumerate(order)}

    def term(k):
        a, b = mine[k]
        return a + b

    far_term = term(4).astype(BF)
    got = along_z(far_term[:half], 1)
    got_dn = along_z(far_term[half:], -1)
    pad = jnp.zeros((half, fw), BF)
    got = jnp.concatenate([got, pad], axis=0)
    got_dn = jnp.concatenate([pad, got_dn], axis=0)
    for k in (3, 2, 1):
        got = along_z((term(k) + got.astype(F32)).astype(BF), 1)
        got_dn = along_z((term(8 - k) + got_dn.astype(F32)).astype(BF), -1)
    slot_grad = (term(0) + got.astype(F32) + got_dn.astype(F32)).astype(BF)

    w_gate, w_up, w_down = weight_grads(
        blocks,
        first + last,
        first_at + [(r + len(first), lane, s) for r, lane, s in last_at],
        backs,
        hidden,
    )

    returned = over_sp(slot_grad.reshape(experts, capacity, fw)).reshape(slots, fw)
    mixed = dot(hot_any, returned, 1, 0).astype(BF)
    th = tokens // 2
    mu1, md1 = along_z(mixed, 1), along_z(mixed, -1)
    mu2, md2 = along_z(mu1, 1), along_z(md1, -1)
    mu3, md3 = along_z(mu2, 1), along_z(md2, -1)
    m4 = jnp.concatenate([along_z(mu3[:th], 1), along_z(md3[th:], -1)], axis=0)
    stack_a = jnp.stack([mixed, mu1, md1, mu2, md2])
    stack_b = jnp.stack([mu3, md3, m4])
    stacks = [stack_a, stack_b, partner(stack_a), partner(stack_b)]
    at = []
    for o in (0, 8):
        r = 0 if o == 0 else 2
        at += [(r, i, o + k) for i, k in enumerate((0, 7, 1, 6, 2))]
        at += [(r + 1, i, o + k) for i, k in enumerate((5, 3, 4))]
    resid, head_grad = residual_grad(
        blocks, stacks, at, residual_mid, inverse, norm_gain[None, :], out_grad, out_proj
    )

    running = jnp.cumsum(log_decay[:, 0])
    total = running[-1]
    t_hi = total.astype(BF)
    t_lo = (total - t_hi.astype(F32)).astype(BF)
    lane = jnp.arange(fw)[None, :]
    extra = jnp.where(lane == 0, t_hi, jnp.where(lane == 1, t_lo, jnp.zeros((), BF)))
    extra = jnp.broadcast_to(extra, (8, fw))
    ret_send = jnp.concatenate([retention_out, extra], axis=0)
    ret_all = over_sp(jnp.broadcast_to(ret_send[None], (16,) + ret_send.shape))
    totals = ret_all[:, tokens, 0].astype(F32) + ret_all[:, tokens, 1].astype(F32)
    ret_rows = ret_all[:, :tokens].reshape(16 * tokens, fw)

    queries = query_rows.astype(F32)
    keys = key_rows.astype(F32)
    values = value_rows.astype(F32)
    key_scale = float(fw) ** (-0.5)
    from_start = jnp.exp(running)[:, None]
    to_end = jnp.exp(running[-1] - running)[:, None]
    causal = pos[:, None] >= pos[None, :]
    spread = jnp.where(causal, running[:, None] - running[None, :], 0.0)
    weights = jnp.where(causal, jnp.exp(spread), 0.0)

    local_state = dot(from_start * queries, head_grad, 0, 0)
    states = over_sp(local_state.astype(BF).reshape(16, 16, fw))
    cum = jnp.cumsum(totals)
    si = jnp.arange(16)
    later_than = si[None, :] > si[:, None]
    gap = jnp.where(later_than, (cum - totals)[None, :] - cum[:, None], 0.0)
    mix = jnp.where(later_than, jnp.exp(gap), 0.0)
    later = jnp.sum(mix[:, :, None, None] * states.astype(F32)[None], axis=1)
    later_state = over_sp(later.astype(BF)).reshape(fw, fw).astype(F32)

    resid_all = over_sp(resid).reshape(16 * tokens, fw)
    proj_grad = dot(resid_all, ret_rows, 0, 0)

    entry = entry_state[0, 0]
    grad_scores = dot(head_grad, values, 1, 1) * weights
    key_scores = dot(queries, keys, 1, 1) * weights
    query_grad = key_scale * (dot(grad_scores, keys, 1, 0) + from_start * dot(head_grad, entry, 1, 1))
    key_grad = key_scale * (dot(grad_scores, queries, 0, 0) + to_end * dot(values, later_state, 1, 1))
    value_grad = key_scale * (dot(key_scores, head_grad, 0, 0) + to_end * dot(keys, later_state, 1, 0))
    return (
        w_gate[None],
        w_up[None],
        w_down[None],
        proj_grad,
        query_grad.astype(BF),
        key_grad.astype(BF),
        value_grad.astype(BF),
    )


def solution(mesh):
    torus = Mesh(mesh.devices.reshape(4, 4, 8, 2), ("y", "x", "z", "c"))
    in_specs = (
        P(SP, None),
        P(SP, None),
        P(),
        P(SP, None),
        P(SP, None),
        P(SP, None, TP),
        P(SP, None, TP),
        P(SP, TP, None),
        P(TP, None),
        P(SP, TP),
        P(SP, TP),
        P(SP, TP),
        P(SP, TP),
        P(SP, TP),
        P(SP, TP, None, None),
    )
    out_specs = (
        P(SP, None, TP),
        P(SP, None, TP),
        P(SP, TP, None),
        P(SP, TP),
        P(SP, TP),
        P(SP, TP),
        P(SP, TP),
    )
    return jax.shard_map(local, mesh=torus, in_specs=in_specs, out_specs=out_specs, check_vma=False)
```
